256 devices in a mesh: ep: 16 (over y, x), tp: 16 (over z, core).
Axes of the slice: x: 4, y: 4, z: 8, core: 2. Of those that a mesh axis runs over, the one named last changes fastest.
Arguments:
- tokens: bfloat16 [512, 2048], P('ep', 'tp'), may hold values from -80 to 80
- delta_state: float32 [512, 16, 128, 128], P('ep', 'tp'), may hold values from -1.8 to 1.8
- mix_gain: bfloat16 [2048], replicated, may hold values from 0.099609375 to 1.8984375
- w_query: bfloat16 [2048, 2048], P(None, 'tp'), may hold values from -0.125 to 0.125
- w_key: bfloat16 [2048, 2048], P(None, 'tp'), may hold values from -0.125 to 0.125
- w_value: bfloat16 [2048, 2048], P(None, 'tp'), may hold values from -0.125 to 0.125
- w_outgate: bfloat16 [2048, 2048], P(None, 'tp'), may hold values from -0.125 to 0.125
- w_beta: bfloat16 [2048, 16], P(None, 'tp'), may hold values from -0.125 to 0.125
- w_decay: bfloat16 [2048, 16], P(None, 'tp'), may hold values from -0.125 to 0.125
- decay_scale: float32 [16], P('tp'), may hold values from 0.05 to 1.5
- decay_bias: float32 [16], P('tp'), may hold values from -1.5 to 1.5
- head_gain: bfloat16 [128], replicated, may hold values from 0.099609375 to 1.8984375
- w_output: bfloat16 [2048, 2048], P('tp'), may hold values from -0.125 to 0.125
- ffn_gain: bfloat16 [2048], replicated, may hold values from 0.099609375 to 1.8984375
- route_ids: int32 [512, 6], P('ep'), may hold values from 0 to 255, all different within a row; in each aligned block of 32 rows (0 to 31, 32 to 63, ...) at most 2 rows name the same one
- route_weights: float32 [512, 6], P('ep'), may hold values from 0.2 to 1.2
- expert_gate: bfloat16 [256, 2048, 512], P(('ep', 'tp')), may hold values from -0.125 to 0.125
- expert_up: bfloat16 [256, 2048, 512], P(('ep', 'tp')), may hold values from -0.125 to 0.125
- expert_down: bfloat16 [256, 512, 2048], P(('ep', 'tp')), may hold values from -0.25 to 0.25
- shared_gate: bfloat16 [2048, 512], P(None, 'tp'), may hold values from -0.125 to 0.125
- shared_up: bfloat16 [2048, 512], P(None, 'tp'), may hold values from -0.125 to 0.125
- shared_down: bfloat16 [512, 2048], P('tp'), may hold values from -0.25 to 0.25
Outputs:
- layer_out: bfloat16 [512, 2048], P('ep', 'tp')
- new_state: float32 [512, 16, 128, 128], P('ep', 'tp')
The draws below stay inside these ranges and needn't reach their ends.
Inputs may be any that keep to these rules, and one draw needn't show every extreme that they name: `route_ids`: each row names 6 different experts. In each aligned block of 32 rows (the sequences of one index of ep) no expert is named by more than 2 rows, and in every draw some expert is named by exactly 2 rows of some block.
All inputs are finite; a program needn't handle non-finite values.
Results may differ from the reference program's by a relative error of at most 0.013.
Values may be sent and summed in bfloat16 or wider, within the bound.
A program may use at most 64 MiB of HBM per device.

```python
import math
import jax
import jax.numpy as jnp
import numpy as np
from jax import lax

D = 2048
HEADS = 16
DK = 128
DV = 128
FE = 512
FS = 512
TOP_K = 6
SEQ_GRP = 32
SEQS = 512
EXPERTS = 256
CAP = 2
N_EP = 16


def draw_tokens(key, part):
    subkeys = jax.random.split(key, 3)
    scale_low = 0.3
    scale_high = 3.0
    base_draw = jnp.clip(jax.random.normal(subkeys[0], (SEQS, D), jnp.float32), -6.0, 6.0)
    row_scales = jnp.exp(jax.random.uniform(subkeys[1], (SEQS, 1), jnp.float32, math.log(scale_low), math.log(scale_high)))
    col_scales = 3.0 ** (jnp.arange(D, dtype=jnp.float32) / D)
    col_scales = col_scales[None, :] * jax.random.uniform(subkeys[2], (1, D), jnp.float32, 0.6, 1.4)
    return (base_draw * row_scales * col_scales).astype(jnp.bfloat16)


def levels(own_key, shape, pieces, low, largest):
    def one(axis_at, shards_of):
        steps = jax.random.uniform(jax.random.fold_in(jax.random.fold_in(own_key, 6), axis_at), (shards_of,), jnp.float32, low / len(pieces), largest / len(pieces))
        return jnp.repeat(jnp.exp(steps), shape[axis_at] // shards_of).reshape((-1,) + (1,) * (len(shape) - axis_at - 1))

    gain = one(*pieces[0])
    for cut in pieces[1:]:
        gain = gain * one(*cut)
    return gain


def routed_block(own_key, own, number, rows, number_of, top, most, skew):
    sequence = jax.random.permutation(own_key, number_of)
    packed, common = portions_of(number_of, rows * top, most, skew, True), portions_of(number_of, rows * top, most, skew, False)
    places = jnp.arange(number_of)

    def named(sizes, offset_by):
        used = int((sizes > 0).sum())
        fixed = max(1, used // 4)
        passed = fixed + (places - fixed + offset_by * (used - fixed)) % max(1, number_of - fixed)
        return jnp.zeros((number_of,), jnp.int32).at[sequence[jnp.where(places < fixed, places, passed)]].set(jnp.asarray(sizes, jnp.int32))

    sizes = jnp.where(number % 4 == 0, named(packed, number // 4), named(common, number - number // 4 - 1))
    mixed = jax.random.permutation(jax.random.fold_in(own, 3), number_of)
    source_of, taker = mixed[0:number_of // 2 * 2:2], mixed[1:number_of // 2 * 2:2]
    slack = jnp.minimum(sizes[source_of] - 1, most - sizes[taker]) // 2
    slack = jnp.where((source_of == sequence[0]) | (taker == sequence[0]) | (sizes[taker] == 0), 0, jnp.maximum(slack, 0))
    passed = jax.random.randint(jax.random.fold_in(own, 4), (number_of // 2,), 0, 1 << 20) % (slack + 1)
    sizes = sizes.at[source_of].add(-passed).at[taker].add(passed)
    members = jnp.searchsorted(jnp.cumsum(sizes), jnp.arange(rows * top), side="right").astype(jnp.int32)
    listing = members.reshape(top, rows).T
    listing = listing[jax.random.permutation(jax.random.fold_in(own, 1), rows)]
    offset_by = jax.random.randint(jax.random.fold_in(own, 2), (rows, 1), 0, top)
    return jnp.take_along_axis(listing, (jnp.arange(top)[None, :] + offset_by) % top, axis=1)


def portions_of(number_of, total, most, skew, full):
    loads = [(1 << 20) // math.isqrt(rank ** skew) + 1 for rank in range(1, number_of + 1)]
    largest = most if full else min(most, max(-(-total // number_of), total * loads[0] // sum(loads)))
    least = 1 if total - largest >= number_of - 1 else 0
    given, surplus = [largest] + [least] * (number_of - 1), total - largest - least * (number_of - 1)
    while surplus > 0:
        movable = [i for i in range(1, number_of) if given[i] < largest] or [i for i in range(1, number_of) if given[i] < most]
        whole, budget = sum([loads[i] for i in movable]), surplus
        for i in movable:
            more = min(most - given[i], max(1, budget * loads[i] // whole), surplus)
            given[i] = given[i] + more
            surplus = surplus - more
    return np.array(given)


def centred(stream_key, extent, width, reach, pieces=(), kind=jnp.bfloat16):
    drawn = width * jax.random.normal(stream_key, extent, jnp.float32)
    if pieces:
        drawn = drawn * levels(stream_key, extent, pieces, -0.22, 0.18)
    return jnp.clip(drawn, -reach, reach).astype(kind)


def setup_inputs(seed: int = 0) -> dict:
    arg_keys = jax.random.split(jax.random.key(seed), 23)
    tokens = draw_tokens(jax.random.fold_in(arg_keys[22], 71), 0)
    delta_state = centred(arg_keys[1], (SEQS, HEADS, DK, DV), 0.3, 1.8, ((0, 16), (1, 16)), jnp.float32)
    mix_gain = jnp.clip(1.0 + 0.18 * jax.random.normal(arg_keys[2], (D,), jnp.float32), 0.099609375, 1.8984375).astype(jnp.bfloat16)
    w_query = centred(arg_keys[3], (D, HEADS * DK), D ** -0.5, 0.125, ((1, 16),))
    w_key = centred(arg_keys[4], (D, HEADS * DK), D ** -0.5, 0.125, ((1, 16),))
    w_value = centred(arg_keys[5], (D, HEADS * DV), D ** -0.5, 0.125, ((1, 16),))
    w_outgate = centred(arg_keys[6], (D, HEADS * DV), D ** -0.5, 0.125, ((1, 16),))
    w_beta = centred(arg_keys[7], (D, HEADS), D ** -0.5, 0.125, ((1, 16),))
    w_decay = centred(arg_keys[8], (D, HEADS), D ** -0.5, 0.125, ((1, 16),))
    decay_scale = jnp.clip(jnp.exp(math.log(1.5) - 3.4011974 * jax.random.uniform(arg_keys[9], (HEADS,), jnp.float32) ** levels(arg_keys[9], (HEADS,), ((0, 16),), -0.2, 0.2)), 0.05, 1.5)
    decay_bias = jnp.clip(jax.random.uniform(arg_keys[10], (HEADS,), jnp.float32, -1.5, 1.5) * levels(arg_keys[10], (HEADS,), ((0, 16),), -0.4, 0.0), -1.5, 1.5)
    head_gain = jnp.clip(1.0 + 0.18 * jax.random.normal(arg_keys[11], (DV,), jnp.float32), 0.099609375, 1.8984375).astype(jnp.bfloat16)
    w_output = centred(arg_keys[12], (HEADS * DV, D), (HEADS * DV) ** -0.5, 0.125, ((0, 16),))
    ffn_gain = jnp.clip(1.0 + 0.18 * jax.random.normal(arg_keys[13], (D,), jnp.float32), 0.099609375, 1.8984375).astype(jnp.bfloat16)
    route_ids_keys = jax.random.split(jax.random.fold_in(arg_keys[14], 1), SEQS // SEQ_GRP)
    route_ids_turns = jax.random.permutation(jax.random.fold_in(arg_keys[14], 3), SEQS // SEQ_GRP)
    route_ids = jax.vmap(lambda own, number: routed_block(jax.random.fold_in(arg_keys[14], 2), own, number, SEQ_GRP, EXPERTS, TOP_K, CAP, 2))(route_ids_keys, route_ids_turns).reshape((SEQS, TOP_K))
    route_weights = jnp.clip(0.2 + 1 * jax.random.uniform(arg_keys[15], (SEQS, TOP_K), jnp.float32) ** levels(arg_keys[15], (SEQS, TOP_K), ((0, 16),), -0.2, 0.2), 0.2, 1.2)
    expert_gate = centred(arg_keys[16], (EXPERTS, D, FE), D ** -0.5, 0.125, ((0, 256),))
    expert_up = centred(arg_keys[17], (EXPERTS, D, FE), D ** -0.5, 0.125, ((0, 256),))
    expert_down = centred(arg_keys[18], (EXPERTS, FE, D), FE ** -0.5, 0.25, ((0, 256),))
    shared_gate = centred(arg_keys[19], (D, FS), D ** -0.5, 0.125, ((1, 16),))
    shared_up = centred(arg_keys[20], (D, FS), D ** -0.5, 0.125, ((1, 16),))
    shared_down = centred(arg_keys[21], (FS, D), FS ** -0.5, 0.25, ((0, 16),))
    return {"tokens": tokens, "delta_state": delta_state, "mix_gain": mix_gain, "w_query": w_query, "w_key": w_key, "w_value": w_value, "w_outgate": w_outgate, "w_beta": w_beta, "w_decay": w_decay, "decay_scale": decay_scale, "decay_bias": decay_bias, "head_gain": head_gain, "w_output": w_output, "ffn_gain": ffn_gain, "route_ids": route_ids, "route_weights": route_weights, "expert_gate": expert_gate, "expert_up": expert_up, "expert_down": expert_down, "shared_gate": shared_gate, "shared_up": shared_up, "shared_down": shared_down}


epsilon = 1e-06

def rms_norm(values, gain_vector):
    squares = lax.optimization_barrier(jnp.mean(values * values, axis=-1, keepdims=True))
    return values * lax.rsqrt(squares + epsilon) * gain_vector.astype(jnp.float32)

def unit_rows(values):
    return values * lax.rsqrt(lax.optimization_barrier(jnp.sum(values * values, axis=-1, keepdims=True)) + epsilon)

def reference(tokens, delta_state, mix_gain, w_query, w_key, w_value, w_outgate, w_beta, w_decay, decay_scale, decay_bias, head_gain, w_output, ffn_gain, route_ids, route_weights, expert_gate, expert_up, expert_down, shared_gate, shared_up, shared_down):
    rows_count = tokens.shape[0]
    resid_in = tokens.astype(jnp.float32)
    normed_mix = rms_norm(resid_in, mix_gain).astype(jnp.bfloat16)

    def project(weight):
        result = jnp.dot(normed_mix, weight, preferred_element_type=jnp.float32)
        result = lax.optimization_barrier(result.astype(jnp.bfloat16)).astype(jnp.float32)
        return result.reshape(rows_count, HEADS, -1)
    query_unit = unit_rows(project(w_query)) * DK ** (-0.5)
    key_unit = unit_rows(project(w_key))
    values_new = project(w_value)
    out_gate = project(w_outgate)
    beta_gate = jax.nn.sigmoid(jnp.dot(normed_mix, w_beta, preferred_element_type=jnp.float32))
    decay_input = jnp.dot(normed_mix, w_decay, preferred_element_type=jnp.float32) + decay_bias
    decay_rate = jnp.exp(-decay_scale * jax.nn.softplus(decay_input))
    key_read = jnp.einsum('shk,shkv->shv', key_unit, delta_state)
    written = beta_gate[:, :, None] * key_unit
    kept_state = delta_state - written[:, :, :, None] * key_read[:, :, None, :]
    new_state = decay_rate[:, :, None, None] * kept_state + written[:, :, :, None] * values_new[:, :, None, :]
    state_read = jnp.einsum('shk,shkv->shv', query_unit, new_state)
    gated = (rms_norm(state_read, head_gain) * jax.nn.silu(out_gate)).reshape(rows_count, -1).astype(jnp.bfloat16)
    resid_mid = resid_in + jnp.dot(gated, w_output, preferred_element_type=jnp.float32)
    normed_ffn = rms_norm(resid_mid, ffn_gain).astype(jnp.bfloat16)
    pair_count = rows_count * TOP_K
    flat_ids = route_ids.reshape(pair_count).astype(jnp.int32)
    flat_rows = (jnp.arange(pair_count, dtype=jnp.int32) // TOP_K).astype(jnp.int32)
    flat_weights = route_weights.reshape(pair_count)
    sorted_order = jnp.argsort(flat_ids, stable=True).astype(jnp.int32)
    sorted_ids = flat_ids[sorted_order]
    expert_range = jnp.arange(EXPERTS, dtype=jnp.int32)
    starts = jnp.searchsorted(sorted_ids, expert_range, side='left').astype(jnp.int32)
    finish = jnp.searchsorted(sorted_ids, expert_range, side='right').astype(jnp.int32)
    most_rows = N_EP * CAP

    def one_expert(running, expert):
        places = starts[expert] + jnp.arange(most_rows, dtype=jnp.int32)
        in_range = places < finish[expert]
        chosen = sorted_order[jnp.minimum(places, pair_count - 1).astype(jnp.int32)]
        rows_at = flat_rows[chosen]
        weights_at = jnp.where(in_range, flat_weights[chosen], 0.0)
        inputs = normed_ffn[rows_at]
        gate_part = jnp.dot(inputs, expert_gate[expert], preferred_element_type=jnp.float32)
        up_part = jnp.dot(inputs, expert_up[expert], preferred_element_type=jnp.float32)
        hidden = (jax.nn.silu(gate_part) * up_part).astype(jnp.bfloat16)
        outputs = jnp.dot(hidden, expert_down[expert], preferred_element_type=jnp.float32)
        outputs = lax.optimization_barrier(outputs.astype(jnp.bfloat16)).astype(jnp.float32)
        return (running.at[rows_at].add(weights_at[:, None] * outputs), None)
    routed, _ = lax.scan(one_expert, jnp.zeros((rows_count, D), jnp.float32), expert_range)
    shared_gate_part = jnp.dot(normed_ffn, shared_gate, preferred_element_type=jnp.float32)
    shared_up_part = jnp.dot(normed_ffn, shared_up, preferred_element_type=jnp.float32)
    hidden_shared = (jax.nn.silu(shared_gate_part) * shared_up_part).astype(jnp.bfloat16)
    shared_out = jnp.dot(hidden_shared, shared_down, preferred_element_type=jnp.float32)
    layer_out = (resid_mid + routed + shared_out).astype(jnp.bfloat16)
    return (layer_out, new_state)
```

```python
import jax
import jax.numpy as jnp
from jax import lax
from jax.experimental import pallas as pl
from jax.experimental.pallas import tpu as pltpu
from jax.sharding import PartitionSpec as P

EPS = 1e-06
MESH = pl.DeviceIdType.MESH
BF = jnp.bfloat16
F32 = jnp.float32
NT = (((1,), (1,)), ((), ()))


def silu(v):
    return v * jax.nn.sigmoid(v)


def dot(a, b):
    return jnp.dot(a, b, preferred_element_type=F32)


def dot_nt(a, b):
    return lax.dot_general(a, b, NT, preferred_element_type=F32)


def row(ref):
    return ref[...].astype(F32).reshape(1, -1)


def kernel(
    tokens, state, mix_gain, w_query, w_key, w_value, w_outgate, w_beta, w_decay, decay_scale, decay_bias,
    head_gain, w_output, ffn_gain, ids, weights, e_gate, e_up, e_down, s_gate, s_up, s_down,
    out, new_state,
    tok_all, st, proj_w, wb, wd, dscale, dbias, mgain, hgain, wo, fgain, idv, rwv, eg, eu, ed, sg, su, sd,
    mix_send, mix_recv, disp_send, disp_recv, res_all, back_send, back_recv, sh_send, sh_recv,
    onehot, comb, k_read, q_read, out_v,
    local_sem, send_sem, recv_sem, entered,
):
    n_ep, n_tp = 16, 16
    ep, tp = lax.axis_index("ep"), lax.axis_index("tp")
    me = ep * n_tp + tp
    rows, width = tokens.shape
    dk = state.shape[2]
    top = ids.shape[0]

    barrier = pltpu.get_barrier_semaphore()
    for d in range(1, n_tp):
        pl.semaphore_signal(barrier, inc=1, device_id=(ep, lax.rem(tp + d, n_tp)), device_id_type=MESH)
        pl.semaphore_signal(barrier, inc=1, device_id=(lax.rem(ep + d, n_ep), tp), device_id_type=MESH)

    fetches = []

    def fetch(src, dst):
        copy = pltpu.make_async_copy(src, dst, local_sem.at[len(fetches)])
        fetches.append(copy)
        copy.start()
        return copy

    c_tok = fetch(tokens, tok_all.at[tp])
    c_route = [fetch(ids, idv), fetch(weights, rwv)]
    c_mix = [
        fetch(mix_gain, mgain), fetch(w_beta, wb), fetch(w_decay, wd), fetch(decay_scale, dscale),
        fetch(decay_bias, dbias), fetch(head_gain, hgain), fetch(ffn_gain, fgain),
    ]
    for i, w in enumerate((w_query, w_key, w_value, w_outgate)):
        c_mix.append(fetch(w, proj_w.at[:, pl.ds(i * dk, dk)]))
    c_mix.append(fetch(state.at[:, 0], st))
    c_mix.append(fetch(w_output, wo))
    c_sh = [fetch(s_gate, sg), fetch(s_up, su), fetch(s_down, sd)]
    c_ex = [fetch(e_gate.at[0], eg), fetch(e_up.at[0], eu), fetch(e_down.at[0], ed)]

    def total(ref, count, sem):
        return pltpu.make_async_copy(ref.at[pl.ds(0, count)], ref.at[pl.ds(0, count)], sem)

    def to_row(src, dst, phase, d):
        pltpu.make_async_remote_copy(
            src, dst, send_sem.at[phase], recv_sem.at[phase],
            device_id=(ep, lax.rem(tp + d, n_tp)), device_id_type=MESH,
        ).start()

    far_first = [8, 9, 7, 10, 6, 11, 5, 12, 4, 13, 3, 14, 2, 15, 1]

    c_tok.wait()
    pl.semaphore_wait(barrier, n_ep + n_tp - 2)
    for d in far_first:
        to_row(tok_all.at[tp], tok_all.at[tp], 0, d)
    for d in range(1, n_ep):
        pl.semaphore_signal(entered, inc=1, device_id=(lax.rem(ep + d, n_ep), tp), device_id_type=MESH)

    for c in c_route:
        c.wait()
    slots = 2 * n_ep * n_tp
    lower = (lax.broadcasted_iota(jnp.int32, (rows, rows), 0) < lax.broadcasted_iota(jnp.int32, (rows, rows), 1)).astype(BF)

    def placed(slot):
        expert, seat = slot // 2, lax.rem(slot, 2)
        named = jnp.zeros(slot.shape, F32)
        weight = jnp.zeros(slot.shape, F32)
        for j in range(top):
            hit = idv[j : j + 1, :] == expert
            named = jnp.where(hit, 1.0, named)
            weight = jnp.where(hit, rwv[j : j + 1, :], weight)
        before = dot(named.astype(BF), lower)
        here = (named > 0.5) & (before == seat.astype(F32))
        return here, weight

    here, weight = placed(lax.broadcasted_iota(jnp.int32, (slots, rows), 0))
    onehot[...] = jnp.where(here, 1.0, 0.0).astype(BF)
    weight = jnp.where(here, weight, 0.0).T
    high = weight.astype(BF)
    comb[0:rows, :] = high
    comb[rows : 2 * rows, :] = (weight - high.astype(F32)).astype(BF)
    pair_row = lax.broadcasted_iota(jnp.int32, (rows, rows), 0)
    own_pair = pair_row // 2 == ep
    own_here, own_weight = placed(2 * me + lax.rem(pair_row, 2))
    own_here = own_here & own_pair
    own_onehot = jnp.where(own_here, 1.0, 0.0).astype(BF)
    own_weight = jnp.where(own_here, own_weight, 0.0).T
    own_high = own_weight.astype(BF)
    own_comb = jnp.concatenate([own_high, (own_weight - own_high.astype(F32)).astype(BF)], axis=0)

    for c in c_mix:
        c.wait()
    total(tok_all, n_tp - 1, recv_sem.at[0]).wait()

    def normed_rows(blocks, gain_row):
        values = jnp.concatenate(blocks, axis=1).astype(F32)
        squares = jnp.mean(values * values, axis=1, keepdims=True)
        return (values * lax.rsqrt(squares + EPS) * gain_row).astype(BF)

    normed = normed_rows([tok_all[t] for t in range(n_tp)], row(mgain))
    projected = dot(normed, proj_w[...]).astype(BF).astype(F32)
    query, key, value, gate = (projected[:, i * dk : (i + 1) * dk] for i in range(4))

    def unit(v):
        return v * lax.rsqrt(jnp.sum(v * v, axis=1, keepdims=True) + EPS)

    query = unit(query) * dk ** (-0.5)
    key = unit(key)
    wide = normed.astype(F32)
    beta = jax.nn.sigmoid(jnp.sum(wide * wb[...].astype(F32), axis=1, keepdims=True))
    decay_in = jnp.sum(wide * wd[...].astype(F32), axis=1, keepdims=True) + dbias[0]
    softplus = jnp.maximum(decay_in, 0.0) + jnp.log(1.0 + jnp.exp(-jnp.abs(decay_in)))
    decay = jnp.exp(-dscale[0] * softplus)
    key_t, query_t = key.T, query.T
    for s in range(rows):
        block = st[s]
        k_read[s : s + 1, :] = jnp.sum(block * key_t[:, s : s + 1], axis=0, keepdims=True)
        q_read[s : s + 1, :] = jnp.sum(block * query_t[:, s : s + 1], axis=0, keepdims=True)
    written = beta * (value - decay * k_read[...])
    read = decay * q_read[...] + jnp.sum(query * key, axis=1, keepdims=True) * written
    squares = jnp.mean(read * read, axis=1, keepdims=True)
    gated = (read * lax.rsqrt(squares + EPS) * row(hgain) * silu(gate)).astype(BF)
    partial = dot(gated, wo[...])
    own_partial = jnp.zeros((rows, width), F32)
    for t in range(n_tp):
        piece = partial[:, t * width : (t + 1) * width]
        mix_send[t] = piece.astype(BF)
        own_partial = jnp.where(tp == t, piece, own_partial)
    for d in far_first:
        to_row(mix_send.at[lax.rem(tp + d, n_tp)], mix_recv.at[d - 1], 1, d)

    for s in range(rows):
        st[s] = decay[s : s + 1, :] * st[s] + key_t[:, s : s + 1] * written[s : s + 1, :]
    c_state = pltpu.make_async_copy(st, new_state.at[:, 0], local_sem.at[len(fetches)])
    c_state.start()

    total(mix_recv, n_tp - 1, recv_sem.at[1]).wait()
    mixed = own_partial
    for d in range(n_tp - 1):
        mixed = mixed + mix_recv[d].astype(F32)
    resid = tok_all[tp].astype(F32) + mixed
    resid_b = resid.astype(BF)

    disp_send[...] = dot(onehot[...], resid_b).astype(BF)
    res_all[tp] = resid_b
    pl.semaphore_wait(entered, n_ep - 1)

    @pl.loop(1, n_ep * n_tp, unroll=5)
    def _(d):
        peer = lax.rem(me + d, n_ep * n_tp)
        pltpu.make_async_remote_copy(
            disp_send.at[pl.ds(pl.multiple_of(2 * peer, 2), 2)],
            disp_recv.at[tp, pl.ds(pl.multiple_of(2 * ep, 2), 2)],
            send_sem.at[2], recv_sem.at[2],
            device_id=(peer // n_tp, lax.rem(peer, n_tp)), device_id_type=MESH,
        ).start()

    for d in far_first:
        to_row(res_all.at[tp], res_all.at[tp], 3, d)
    own_disp = dot(own_onehot, resid_b).astype(BF)

    for c in c_ex:
        c.wait()
    pltpu.make_async_copy(back_recv.at[pl.ds(0, slots - 2)], back_recv.at[pl.ds(0, slots - 2)], recv_sem.at[2]).wait()
    fgain_row = row(fgain)
    own_block = lax.broadcasted_iota(jnp.int32, (rows, width), 0) // 2 == ep
    routed_rows = normed_rows(
        [jnp.where(own_block & (tp == t), own_disp, disp_recv[t]) for t in range(n_tp)], fgain_row
    )
    hidden = (silu(dot(routed_rows, eg[...])) * dot(routed_rows, eu[...])).astype(BF)
    results = dot(hidden, ed[...])
    own_back = jnp.zeros((rows, width), F32)
    for t in range(n_tp):
        piece = results[:, t * width : (t + 1) * width]
        back_send[t] = piece.astype(BF)
        own_back = jnp.where(tp == t, piece, own_back)

    @pl.loop(1, n_ep * n_tp, unroll=5)
    def _(d):
        peer = lax.rem(me + d, n_ep * n_tp)
        to_ep, to_tp = peer // n_tp, lax.rem(peer, n_tp)
        pltpu.make_async_remote_copy(
            back_send.at[to_tp, pl.ds(pl.multiple_of(2 * to_ep, 2), 2)],
            back_recv.at[pl.ds(pl.multiple_of(2 * me, 2), 2)],
            send_sem.at[4], recv_sem.at[4],
            device_id=(to_ep, to_tp), device_id_type=MESH,
        ).start()

    for c in c_sh:
        c.wait()
    total(res_all, n_tp - 1, recv_sem.at[3]).wait()
    normed_ffn = normed_rows([res_all[t] for t in range(n_tp)], fgain_row)
    hidden_shared = (silu(dot_nt(normed_ffn, sg[...])) * dot_nt(normed_ffn, su[...])).astype(BF)
    shared = dot(hidden_shared, sd[...])
    own_shared = jnp.zeros((rows, width), F32)
    for t in range(n_tp):
        piece = shared[:, t * width : (t + 1) * width]
        sh_send[t] = piece.astype(BF)
        own_shared = jnp.where(tp == t, piece, own_shared)
    for d in far_first:
        to_row(sh_send.at[lax.rem(tp + d, n_tp)], sh_recv.at[d - 1], 5, d)

    own_routed = dot(own_comb, own_back.astype(BF))
    final = resid + own_shared + own_routed[0:rows] + own_routed[rows : 2 * rows]
    total(sh_recv, n_tp - 1, recv_sem.at[5]).wait()
    for d in range(n_tp - 1):
        final = final + sh_recv[d].astype(F32)
    pltpu.make_async_copy(back_recv.at[pl.ds(0, slots - 2)], back_recv.at[pl.ds(0, slots - 2)], recv_sem.at[4]).wait()
    own_rows = lax.broadcasted_iota(jnp.int32, (slots, width), 0) // 2 == me
    arrived = jnp.where(own_rows, jnp.zeros((slots, width), BF), back_recv[...])
    routed = dot(comb[...], arrived)
    out_v[...] = (final + routed[0:rows] + routed[rows : 2 * rows]).astype(BF)
    c_out = pltpu.make_async_copy(out_v, out, local_sem.at[len(fetches) + 1])
    c_out.start()

    for phase, ref in ((0, tok_all), (1, mix_recv), (3, res_all), (5, sh_recv)):
        total(ref, n_tp - 1, send_sem.at[phase]).wait()
    for phase in (2, 4):
        pltpu.make_async_copy(
            back_recv.at[pl.ds(0, slots - 2)], back_recv.at[pl.ds(0, slots - 2)], send_sem.at[phase]
        ).wait()
    c_state.wait()
    c_out.wait()


def body(
    tokens, delta_state, mix_gain, w_query, w_key, w_value, w_outgate, w_beta, w_decay, decay_scale, decay_bias,
    head_gain, w_output, ffn_gain, route_ids, route_weights, expert_gate, expert_up, expert_down, shared_gate,
    shared_up, shared_down,
):
    rows, width = tokens.shape
    n_ep, n_tp = lax.axis_size("ep"), lax.axis_size("tp")
    model, dk = w_query.shape
    top = route_ids.shape[1]
    fe = expert_gate.shape[2]
    fs = shared_gate.shape[1]
    slots = 2 * n_ep * n_tp
    block = (n_tp, rows, width)
    V = pltpu.VMEM
    dma = pltpu.SemaphoreType.DMA
    return pl.pallas_call(
        kernel,
        out_shape=(
            jax.ShapeDtypeStruct(tokens.shape, tokens.dtype),
            jax.ShapeDtypeStruct(delta_state.shape, delta_state.dtype),
        ),
        in_specs=[pl.BlockSpec(memory_space=pl.ANY)] * 22,
        out_specs=(pl.BlockSpec(memory_space=pl.ANY),) * 2,
        scratch_shapes=[
            V(block, BF),
            V((rows, dk, dk), F32),
            V((model, 4 * dk), BF),
            V((1, model), BF),
            V((1, model), BF),
            pltpu.SMEM((1,), F32),
            pltpu.SMEM((1,), F32),
            V((model,), BF),
            V((dk,), BF),
            V((dk, model), BF),
            V((model,), BF),
            V((top, rows), jnp.int32),
            V((top, rows), F32),
            V((model, fe), BF),
            V((model, fe), BF),
            V((fe, model), BF),
            V((fs, model), BF),
            V((fs, model), BF),
            V((fs, model), BF),
            V(block, BF),
            V((n_tp - 1, rows, width), BF),
            V((slots, width), BF),
            V(block, BF),
            V(block, BF),
            V(block, BF),
            V((slots, width), BF),
            V(block, BF),
            V((n_tp - 1, rows, width), BF),
            V((slots, rows), BF),
            V((2 * rows, slots), BF),
            V((rows, dk), F32),
            V((rows, dk), F32),
            V((rows, width), BF),
            dma((24,)),
            dma((6,)),
            dma((6,)),
            pltpu.SemaphoreType.REGULAR,
        ],
        compiler_params=pltpu.CompilerParams(collective_id=0, has_side_effects=True),
        name="layer",
    )(
        tokens, delta_state, mix_gain, w_query, w_key, w_value, w_outgate, w_beta.T, w_decay.T, decay_scale,
        decay_bias, head_gain, w_output, ffn_gain, route_ids.T, route_weights.T, expert_gate, expert_up, expert_down,
        shared_gate.T, shared_up.T, shared_down,
    )


def solution(mesh):
    return jax.shard_map(
        body,
        mesh=mesh,
        in_specs=(
            P("ep", "tp"),
            P("ep", "tp", None, None),
            P(),
            P(None, "tp"),
            P(None, "tp"),
            P(None, "tp"),
            P(None, "tp"),
            P(None, "tp"),
            P(None, "tp"),
            P("tp"),
            P("tp"),
            P(),
            P("tp", None),
            P(),
            P("ep", None),
            P("ep", None),
            P(("ep", "tp"), None, None),
            P(("ep", "tp"), None, None),
            P(("ep", "tp"), None, None),
            P(None, "tp"),
            P(None, "tp"),
            P("tp", None),
        ),
        out_specs=(P("ep", "tp"), P("ep", "tp", None, None)),
        check_vma=False,
    )
```

```python
import jax
import jax.numpy as jnp
from jax import lax
from jax.experimental import pallas as pl
from jax.experimental.pallas import tpu as pltpu
from jax.sharding import PartitionSpec as P

EPS = 1e-06
MESH = pl.DeviceIdType.MESH
BF = jnp.bfloat16
F32 = jnp.float32
NT = (((1,), (1,)), ((), ()))


def silu(v):
    return v * jax.nn.sigmoid(v)


def dot(a, b):
    return jnp.dot(a, b, preferred_element_type=F32)


def dot_nt(a, b):
    return lax.dot_general(a, b, NT, preferred_element_type=F32)


def row(ref):
    return ref[...].astype(F32).reshape(1, -1)


ZO = (4, 3, 5, 2, 6, 1, 7, 0)
RO = (2, 1, 3, 0)


def ring(i, n):
    half = i // 2
    return n // 2 + half - lax.rem(i, 2) * (2 * half + 1)


def kernel(
    tokens, state, mix_gain, w_query, w_key, w_value, w_outgate, w_beta, w_decay, decay_scale, decay_bias,
    head_gain, w_output, ffn_gain, ids, weights, e_gate, e_up, e_down, s_gate, s_up, s_down,
    out, st,
    tok_all, st_split, proj_w, wb, wd, dscale, dbias, mgain, hgain, wo, fgain, fgain8, idv, rwv, eg, eu, ed, sg, su, sd,
    mix_send, mix_recv, disp_send, disp_recv, res_all, back_send, back_recv, sh_send, sh_recv,
    onehot, comb, k_read, q_read, sized,
    local_sem, send_sem, recv_sem, entered,
):
    n_ep, n_tp = 16, 16
    ep, tp = lax.axis_index("ep"), lax.axis_index("tp")
    me = ep * n_tp + tp
    y, x = ep // 4, lax.rem(ep, 4)
    z, core = tp // 2, lax.rem(tp, 2)
    rows, width = tokens.shape
    dk = state.shape[2]
    top = ids.shape[0]
    slots = 2 * n_ep * n_tp
    wide2 = 2 * width

    barrier = pltpu.get_barrier_semaphore()
    for d in range(1, n_tp):
        pl.semaphore_signal(barrier, inc=1, device_id=(ep, lax.rem(tp + d, n_tp)), device_id_type=MESH)
        pl.semaphore_signal(barrier, inc=1, device_id=(lax.rem(ep + d, n_ep), tp), device_id_type=MESH)

    fetches = []

    def fetch(src, dst):
        copy = pltpu.make_async_copy(src, dst, local_sem.at[len(fetches)])
        fetches.append(copy)
        copy.start()
        return copy

    c_tok = fetch(tokens, tok_all.at[tp])
    c_route = [fetch(ids, idv), fetch(weights, rwv)]
    c_state = fetch(state.at[:, 0], st)
    c_mix = [
        fetch(mix_gain, mgain), fetch(w_beta, wb), fetch(w_decay, wd), fetch(decay_scale, dscale),
        fetch(decay_bias, dbias), fetch(head_gain, hgain), fetch(ffn_gain, fgain),
    ]
    for i, w in enumerate((w_query, w_key, w_value, w_outgate)):
        c_mix.append(fetch(w, proj_w.at[:, pl.ds(i * dk, dk)]))
    c_mix.append(fetch(w_output, wo))
    c_sh = [fetch(s_gate, sg), fetch(s_up, su), fetch(s_down, sd)]
    c_ex = []
    z_from = [lax.rem(z + 8 - ZO[a], 8) for a in range(8)]
    z_to = [lax.rem(z + ZO[a], 8) for a in range(8)]
    for a in range(8):
        here, there = pl.ds(a * wide2, wide2), pl.ds(pl.multiple_of(z_from[a] * wide2, wide2), wide2)
        c_ex += [fetch(e_gate.at[0, there], eg.at[here]), fetch(e_up.at[0, there], eu.at[here])]
        there = pl.ds(pl.multiple_of(z_to[a] * wide2, wide2), wide2)
        c_ex.append(fetch(e_down.at[0, :, there], ed.at[:, here]))

    def total(ref, count, sem):
        return pltpu.make_async_copy(ref.at[pl.ds(0, count)], ref.at[pl.ds(0, count)], sem)

    def to_row(src, dst, phase, d):
        pltpu.make_async_remote_copy(
            src, dst, send_sem.at[phase], recv_sem.at[phase],
            device_id=(ep, lax.rem(tp + d, n_tp)), device_id_type=MESH,
        ).start()

    far_first = [8, 9, 7, 10, 6, 11, 5, 12, 4, 13, 3, 14, 2, 15, 1]

    c_tok.wait()
    pl.semaphore_wait(barrier, n_ep + n_tp - 2)
    for d in far_first:
        to_row(tok_all.at[tp], tok_all.at[tp], 0, d)
    for d in range(1, n_ep):
        pl.semaphore_signal(entered, inc=1, device_id=(lax.rem(ep + d, n_ep), tp), device_id_type=MESH)

    for c in c_route:
        c.wait()
    lower = (
        lax.broadcasted_iota(jnp.int32, (rows, rows), 0) < lax.broadcasted_iota(jnp.int32, (rows, rows), 1)
    ).astype(BF)

    def placed(expert, seat):
        named = jnp.zeros(expert.shape, F32)
        weight = jnp.zeros(expert.shape, F32)
        for j in range(top):
            hit = idv[j : j + 1, :] == expert
            named = jnp.where(hit, 1.0, named)
            weight = jnp.where(hit, rwv[j : j + 1, :], weight)
        before = dot(named.astype(BF), lower)
        return (named > 0.5) & (before == seat.astype(F32)), weight

    slot = lax.broadcasted_iota(jnp.int32, (slots, rows), 0)
    pair = slot // 2
    seat = slot - 2 * pair
    off_x, off_y = ring(pair % 4, 4), ring((pair // 4) % 4, 4)
    off_z, slot_core = ring(pair // 32, 8), (pair // 16) % 2
    far_ep = ((y + off_y) % 4) * 4 + (x + off_x) % 4
    here, _ = placed(far_ep * n_tp + ((z + off_z) % 8) * 2 + slot_core, seat)
    onehot[...] = jnp.where(here, 1.0, 0.0).astype(BF)
    here, weight = placed(far_ep * n_tp + ((z + 8 - off_z) % 8) * 2 + slot_core, seat)
    weight = jnp.where(here, weight, 0.0).T
    high = weight.astype(BF)
    comb[0:rows, :] = high
    comb[rows : 2 * rows, :] = (weight - high.astype(F32)).astype(BF)
    pair_row = lax.broadcasted_iota(jnp.int32, (rows, rows), 0)
    own_here, own_weight = placed(jnp.full((rows, rows), 0, jnp.int32) + me, pair_row % 2)
    own_here = own_here & (pair_row // 2 == n_ep - 1)
    own_onehot = jnp.where(own_here, 1.0, 0.0).astype(BF)
    own_weight = jnp.where(own_here, own_weight, 0.0).T
    own_high = own_weight.astype(BF)
    own_comb = jnp.concatenate([own_high, (own_weight - own_high.astype(F32)).astype(BF)], axis=0)

    c_state.wait()

    @pl.loop(0, rows, unroll=4)
    def _(s):
        block = st[s]
        high = block.astype(BF)
        st_split[s, 0:dk, :] = high
        st_split[s, dk : 2 * dk, :] = (block - high.astype(F32)).astype(BF)

    for c in c_mix:
        c.wait()
    fgain_row = row(fgain)
    for i in range(8):
        fgain8[i : i + 1, :] = fgain_row[:, i * wide2 : (i + 1) * wide2]
    total(tok_all, n_tp - 1, recv_sem.at[0]).wait()

    def normed_rows(blocks, gain_row):
        values = jnp.concatenate(blocks, axis=1).astype(F32)
        squares = jnp.mean(values * values, axis=1, keepdims=True)
        return (values * lax.rsqrt(squares + EPS) * gain_row).astype(BF)

    normed = normed_rows([tok_all[t] for t in range(n_tp)], row(mgain))
    projected = dot(normed, proj_w[...]).astype(BF).astype(F32)
    query, key, value, gate = (projected[:, i * dk : (i + 1) * dk] for i in range(4))

    def unit(v):
        return v * lax.rsqrt(jnp.sum(v * v, axis=1, keepdims=True) + EPS)

    query = unit(query) * dk ** (-0.5)
    key = unit(key)

    def two_parts(v):
        high = v.astype(BF).astype(F32)
        return high, v - high

    k_high, k_low = two_parts(key)
    q_high, q_low = two_parts(query)
    for s0 in range(0, rows, 8):
        some = slice(s0, s0 + 8)
        left = jnp.concatenate([k_high[some], q_high[some], k_low[some], q_low[some]], axis=0).astype(BF)
        left = jnp.concatenate([left, left], axis=1)
        for i in range(8):
            s = s0 + i
            both = dot(left, st_split[s])
            k_read[s : s + 1, :] = both[i : i + 1] + both[16 + i : 17 + i]
            q_read[s : s + 1, :] = both[8 + i : 9 + i] + both[24 + i : 25 + i]
    wide = normed.astype(F32)
    beta = jax.nn.sigmoid(jnp.sum(wide * wb[...].astype(F32), axis=1, keepdims=True))
    decay_in = jnp.sum(wide * wd[...].astype(F32), axis=1, keepdims=True) + dbias[0]
    softplus = jnp.maximum(decay_in, 0.0) + jnp.log(1.0 + jnp.exp(-jnp.abs(decay_in)))
    decay = jnp.exp(-dscale[0] * softplus)
    written = beta * (value - decay * k_read[...])
    read = decay * q_read[...] + jnp.sum(query * key, axis=1, keepdims=True) * written
    squares = jnp.mean(read * read, axis=1, keepdims=True)
    gated = (read * lax.rsqrt(squares + EPS) * row(hgain) * silu(gate)).astype(BF)
    partial = dot(gated, wo[...])
    own_partial = jnp.zeros((rows, width), F32)
    for t in range(n_tp):
        piece = partial[:, t * width : (t + 1) * width]
        mix_send[t] = piece.astype(BF)
        own_partial = jnp.where(tp == t, piece, own_partial)
    for d in far_first:
        to_row(mix_send.at[lax.rem(tp + d, n_tp)], mix_recv.at[d - 1], 1, d)

    key_t = key.T
    for s in range(rows):
        st[s] = decay[s : s + 1, :] * st[s] + key_t[:, s : s + 1] * written[s : s + 1, :]

    total(mix_recv, n_tp - 1, recv_sem.at[1]).wait()
    mixed = own_partial
    for d in range(n_tp - 1):
        mixed = mixed + mix_recv[d].astype(F32)
    resid = tok_all[tp].astype(F32) + mixed
    resid_b = resid.astype(BF)

    res_all[tp] = resid_b
    disp_send[...] = dot(onehot[...], resid_b).astype(BF).reshape(disp_send.shape)

    def to_all(src, dst, phase, sign):
        to_y = [lax.rem(y + 4 + sign * r, 4) * 4 for r in RO]
        to_x = [lax.rem(x + 4 + sign * r, 4) for r in RO]
        to_ep = [to_y[b] + to_x[e] for b in range(4) for e in range(4)]

        def send(a, c, i, dev_tp):
            seats = pl.ds(2 * i, 2)
            pltpu.make_async_remote_copy(
                src.at[a, c, seats], dst.at[a, core, seats], send_sem.at[phase], recv_sem.at[phase],
                device_id=(to_ep[i], dev_tp), device_id_type=MESH,
            ).start()

        @pl.loop(0, 7)
        def _(a):
            dev_tp = lax.rem(z + ring(a, 8), 8) * 2
            for i in range(16):
                for c in range(2):
                    send(a, c, i, dev_tp + c)

        for i in range(15):
            for c in range(2):
                send(7, c, i, 2 * z + c)
        send(7, 1 - core, 15, 2 * z + 1 - core)

    def all_sent(sem):
        as_many = sized.at[pl.ds(0, slots - 2)]
        return pltpu.make_async_copy(as_many, as_many, sem)

    pl.semaphore_wait(entered, n_ep - 1)
    to_all(disp_send, disp_recv, 2, 1)
    for d in far_first:
        to_row(res_all.at[tp], res_all.at[tp], 3, d)
    own_disp = dot(own_onehot, resid_b).astype(BF)

    for c in c_ex:
        c.wait()
    all_sent(recv_sem.at[2]).wait()
    own_block = lax.broadcasted_iota(jnp.int32, (rows, width), 0) // 2 == n_ep - 1
    blocks = [disp_recv[a, c] for a in range(8) for c in range(2)]
    for c in range(2):
        blocks[14 + c] = jnp.where(own_block & (core == c), own_disp, blocks[14 + c])
    gain_from = jnp.concatenate([fgain8[pl.ds(z_from[a], 1), :] for a in range(8)], axis=1)
    routed_rows = normed_rows(blocks, gain_from)
    hidden = (silu(dot(routed_rows, eg[...])) * dot(routed_rows, eu[...])).astype(BF)
    results = dot(hidden, ed[...])
    for a in range(8):
        for c in range(2):
            back_send[a, c] = results[:, (2 * a + c) * width : (2 * a + c + 1) * width].astype(BF)
    own_back = jnp.where(core == 0, results[:, 14 * width : 15 * width], results[:, 15 * width : 16 * width])
    to_all(back_send, back_recv, 4, -1)

    for c in c_sh:
        c.wait()
    total(res_all, n_tp - 1, recv_sem.at[3]).wait()
    normed_ffn = normed_rows([res_all[t] for t in range(n_tp)], fgain_row)
    hidden_shared = (silu(dot_nt(normed_ffn, sg[...])) * dot_nt(normed_ffn, su[...])).astype(BF)
    shared = dot(hidden_shared, sd[...])
    own_shared = jnp.zeros((rows, width), F32)
    for t in range(n_tp):
        piece = shared[:, t * width : (t + 1) * width]
        sh_send[t] = piece.astype(BF)
        own_shared = jnp.where(tp == t, piece, own_shared)
    for d in far_first:
        to_row(sh_send.at[lax.rem(tp + d, n_tp)], sh_recv.at[d - 1], 5, d)
    own_routed = dot(own_comb, own_back.astype(BF))
    final = resid + own_shared + own_routed[0:rows] + own_routed[rows : 2 * rows]
    total(sh_recv, n_tp - 1, recv_sem.at[5]).wait()
    for d in range(n_tp - 1):
        final = final + sh_recv[d].astype(F32)
    all_sent(recv_sem.at[4]).wait()
    own_rows = lax.broadcasted_iota(jnp.int32, (slots, width), 0) // 2 == (14 + core) * n_ep + n_ep - 1
    arrived = jnp.where(own_rows, jnp.zeros((slots, width), BF), back_recv[...].reshape(slots, width))
    routed = dot(comb[...], arrived)
    out[...] = (final + routed[0:rows] + routed[rows : 2 * rows]).astype(BF)

    for phase, ref in ((0, tok_all), (1, mix_recv), (3, res_all), (5, sh_recv)):
        total(ref, n_tp - 1, send_sem.at[phase]).wait()
    for phase in (2, 4):
        all_sent(send_sem.at[phase]).wait()


def put_out(out_v, st, out, new_state, sem):
    rows = st.shape[0]
    step = rows // 4
    copies = [pltpu.make_async_copy(out_v, out, sem.at[4])]
    for i in range(4):
        some = pl.ds(i * step, step)
        copies.append(pltpu.make_async_copy(st.at[some], new_state.at[some, 0], sem.at[i]))
    for c in copies:
        c.start()
    for c in copies:
        c.wait()


def body(
    tokens, delta_state, mix_gain, w_query, w_key, w_value, w_outgate, w_beta, w_decay, decay_scale, decay_bias,
    head_gain, w_output, ffn_gain, route_ids, route_weights, expert_gate, expert_up, expert_down, shared_gate,
    shared_up, shared_down,
):
    rows, width = tokens.shape
    n_ep, n_tp = lax.axis_size("ep"), lax.axis_size("tp")
    model, dk = w_query.shape
    top = route_ids.shape[1]
    fe = expert_gate.shape[2]
    fs = shared_gate.shape[1]
    slots = 2 * n_ep * n_tp
    block = (n_tp, rows, width)
    spread = (8, 2, rows, width)
    V = pltpu.VMEM
    dma = pltpu.SemaphoreType.DMA
    on_chip = pl.BlockSpec(memory_space=pltpu.VMEM)
    in_hbm = pl.BlockSpec(memory_space=pltpu.HBM)
    out_v, st = pl.pallas_call(
        kernel,
        out_shape=(V(tokens.shape, tokens.dtype), V((rows, dk, dk), F32)),
        in_specs=[in_hbm] * 22,
        out_specs=(on_chip, on_chip),
        scratch_shapes=[
            V(block, BF),
            V((rows, 2 * dk, dk), BF),
            V((model, 4 * dk), BF),
            V((1, model), BF),
            V((1, model), BF),
            pltpu.SMEM((1,), F32),
            pltpu.SMEM((1,), F32),
            V((model,), BF),
            V((dk,), BF),
            V((dk, model), BF),
            V((model,), BF),
            V((8, 2 * width), F32),
            V((top, rows), jnp.int32),
            V((top, rows), F32),
            V((model, fe), BF),
            V((model, fe), BF),
            V((fe, model), BF),
            V((fs, model), BF),
            V((fs, model), BF),
            V((fs, model), BF),
            V(block, BF),
            V((n_tp - 1, rows, width), BF),
            V(spread, BF),
            V(spread, BF),
            V(block, BF),
            V(spread, BF),
            V(spread, BF),
            V(block, BF),
            V((n_tp - 1, rows, width), BF),
            V((slots, rows), BF),
            V((2 * rows, slots), BF),
            V((rows, dk), F32),
            V((rows, dk), F32),
            V((slots, width), BF),
            dma((48,)),
            dma((6,)),
            dma((6,)),
            pltpu.SemaphoreType.REGULAR,
        ],
        compiler_params=pltpu.CompilerParams(
            collective_id=0, has_side_effects=True, vmem_limit_bytes=48 * 1024 * 1024
        ),
        name="layer",
    )(*(v if v.size == 1 else pltpu.with_memory_space_constraint(v, pltpu.HBM) for v in (
        tokens, delta_state, mix_gain, w_query, w_key, w_value, w_outgate, w_beta.T, w_decay.T,
        decay_scale, decay_bias, head_gain, w_output, ffn_gain, route_ids.T,
        route_weights.T, expert_gate, expert_up, expert_down, shared_gate.T, shared_up.T, shared_down,
    )))
    out_v, st = (pltpu.with_memory_space_constraint(v, pltpu.VMEM) for v in (out_v, st))
    return pl.pallas_call(
        put_out,
        out_shape=(
            jax.ShapeDtypeStruct(tokens.shape, tokens.dtype),
            jax.ShapeDtypeStruct(delta_state.shape, delta_state.dtype),
        ),
        in_specs=[on_chip, on_chip],
        out_specs=(in_hbm, in_hbm),
        scratch_shapes=[dma((5,))],
        name="put_out",
    )(out_v, st)


def solution(mesh):
    return jax.shard_map(
        body,
        mesh=mesh,
        in_specs=(
            P("ep", "tp"),
            P("ep", "tp", None, None),
            P(),
            P(None, "tp"),
            P(None, "tp"),
            P(None, "tp"),
            P(None, "tp"),
            P(None, "tp"),
            P(None, "tp"),
            P("tp"),
            P("tp"),
            P(),
            P("tp", None),
            P(),
            P("ep", None),
            P("ep", None),
            P(("ep", "tp"), None, None),
            P(("ep", "tp"), None, None),
            P(("ep", "tp"), None, None),
            P(None, "tp"),
            P(None, "tp"),
            P("tp", None),
        ),
        out_specs=(P("ep", "tp"), P("ep", "tp", None, None)),
        check_vma=False,
    )
```

```python
import jax
import jax.numpy as jnp
from jax import lax
from jax.experimental import pallas as pl
from jax.experimental.pallas import tpu as pltpu
from jax.sharding import PartitionSpec as P

EPS = 1e-06
MESH = pl.DeviceIdType.MESH
BF = jnp.bfloat16
F32 = jnp.float32
NT = (((1,), (1,)), ((), ()))


def silu(v):
    return v * jax.nn.sigmoid(v)


def dot(a, b):
    return jnp.dot(a, b, preferred_element_type=F32)


def dot_nt(a, b):
    return lax.dot_general(a, b, NT, preferred_element_type=F32)


def row(ref):
    return ref[...].astype(F32).reshape(1, -1)


ZO = (4, 3, 5, 2, 6, 1, 7, 0)
RO = (2, 1, 3, 0)


def ring(i, n):
    half = i // 2
    return n // 2 + half - lax.rem(i, 2) * (2 * half + 1)


def kernel(
    tokens, state, mix_gain, w_query, w_key, w_value, w_outgate, w_beta, w_decay, decay_scale, decay_bias,
    head_gain, w_output, ffn_gain, ids, weights, e_gate, e_up, e_down, s_gate, s_up, s_down,
    out, st,
    tok_all, st_split, proj_w, wb, wd, dscale, dbias, mgain, hgain, wo, fgain, fgain8, idv, rwv, eg, eu, ed, sg, su, sd,
    mix_send, mix_recv, disp_send, disp_recv, res_all, back_send, back_recv, sh_send, sh_recv,
    onehot, comb, k_read, q_read, sized,
    local_sem, send_sem, recv_sem, entered,
):
    n_ep, n_tp = 16, 16
    ep, tp = lax.axis_index("ep"), lax.axis_index("tp")
    me = ep * n_tp + tp
    y, x = ep // 4, lax.rem(ep, 4)
    z, core = tp // 2, lax.rem(tp, 2)
    rows, width = tokens.shape
    dk = state.shape[2]
    top = ids.shape[0]
    slots = 2 * n_ep * n_tp
    wide2 = 2 * width

    barrier = pltpu.get_barrier_semaphore()
    far_first = [8, 9, 7, 10, 6, 11, 5, 12, 4, 13, 3, 14, 2, 15, 1]
    for d in far_first:
        pl.semaphore_signal(barrier, inc=1, device_id=(ep, lax.rem(tp + d, n_tp)), device_id_type=MESH)
    for d in far_first:
        pl.semaphore_signal(barrier, inc=1, device_id=(lax.rem(ep + d, n_ep), tp), device_id_type=MESH)

    fetches = []

    def fetch(src, dst):
        copy = pltpu.make_async_copy(src, dst, local_sem.at[len(fetches)])
        fetches.append(copy)
        copy.start()
        return copy

    def fetch_pieces(pieces, whole):
        sem = local_sem.at[len(fetches)]
        for src, dst in pieces:
            pltpu.make_async_copy(src, dst, sem).start()
        fetches.append(pltpu.make_async_copy(whole, whole, sem))
        return fetches[-1]

    c_tok = fetch(tokens, tok_all.at[tp])
    c_route = [fetch(ids, idv), fetch(weights, rwv)]
    c_state = fetch(state.at[:, 0], st)
    c_mix = [
        fetch(mix_gain, mgain), fetch(w_beta, wb), fetch(w_decay, wd), fetch(decay_scale, dscale),
        fetch(decay_bias, dbias), fetch(head_gain, hgain), fetch(ffn_gain, fgain),
    ]
    four = enumerate((w_query, w_key, w_value, w_outgate))
    c_mix.append(fetch_pieces([(w, proj_w.at[:, pl.ds(i * dk, dk)]) for i, w in four], proj_w))
    c_mix.append(fetch(w_output, wo))
    c_sh = [fetch(s_gate, sg), fetch(s_up, su), fetch(s_down, sd)]
    z_from = [lax.rem(z + 8 - ZO[a], 8) for a in range(8)]
    z_to = [lax.rem(z + ZO[a], 8) for a in range(8)]
    here = [pl.ds(a * wide2, wide2) for a in range(8)]
    from_z = [pl.ds(pl.multiple_of(v * wide2, wide2), wide2) for v in z_from]
    to_z = [pl.ds(pl.multiple_of(v * wide2, wide2), wide2) for v in z_to]
    c_ex = [
        fetch_pieces([(e_gate.at[0, from_z[a]], eg.at[here[a]]) for a in range(8)], eg),
        fetch_pieces([(e_up.at[0, from_z[a]], eu.at[here[a]]) for a in range(8)], eu),
        fetch_pieces([(e_down.at[0, :, to_z[a]], ed.at[:, here[a]]) for a in range(8)], ed),
    ]

    def total(ref, count, sem):
        return pltpu.make_async_copy(ref.at[pl.ds(0, count)], ref.at[pl.ds(0, count)], sem)

    def to_row(src, dst, phase, d):
        pltpu.make_async_remote_copy(
            src, dst, send_sem.at[phase], recv_sem.at[phase],
            device_id=(ep, lax.rem(tp + d, n_tp)), device_id_type=MESH,
        ).start()

    c_tok.wait()
    pl.semaphore_wait(barrier, n_ep + n_tp - 2)
    for d in far_first:
        to_row(tok_all.at[tp], tok_all.at[tp], 0, d)
    for d in range(1, n_ep):
        pl.semaphore_signal(entered, inc=1, device_id=(lax.rem(ep + d, n_ep), tp), device_id_type=MESH)

    for c in c_route:
        c.wait()
    lower = (
        lax.broadcasted_iota(jnp.int32, (rows, rows), 0) < lax.broadcasted_iota(jnp.int32, (rows, rows), 1)
    ).astype(BF)

    def placed(expert, seat):
        named = jnp.zeros(expert.shape, F32)
        weight = jnp.zeros(expert.shape, F32)
        for j in range(top):
            hit = idv[j : j + 1, :] == expert
            named = jnp.where(hit, 1.0, named)
            weight = jnp.where(hit, rwv[j : j + 1, :], weight)
        before = dot(named.astype(BF), lower)
        return (named > 0.5) & (before == seat.astype(F32)), weight

    slot = lax.broadcasted_iota(jnp.int32, (slots, rows), 0)
    pair = slot // 2
    seat = slot - 2 * pair
    off_x, off_y = ring(pair % 4, 4), ring((pair // 4) % 4, 4)
    off_z, slot_core = ring(pair // 32, 8), (pair // 16) % 2
    far_ep = ((y + off_y) % 4) * 4 + (x + off_x) % 4
    here, _ = placed(far_ep * n_tp + ((z + off_z) % 8) * 2 + slot_core, seat)
    onehot[...] = jnp.where(here, 1.0, 0.0).astype(BF)
    here, weight = placed(far_ep * n_tp + ((z + 8 - off_z) % 8) * 2 + slot_core, seat)
    weight = jnp.where(here, weight, 0.0).T
    high = weight.astype(BF)
    comb[0:rows, :] = high
    comb[rows : 2 * rows, :] = (weight - high.astype(F32)).astype(BF)
    pair_row = lax.broadcasted_iota(jnp.int32, (rows, rows), 0)
    own_here, own_weight = placed(jnp.full((rows, rows), 0, jnp.int32) + me, pair_row % 2)
    own_here = own_here & (pair_row // 2 == n_ep - 1)
    own_onehot = jnp.where(own_here, 1.0, 0.0).astype(BF)
    own_weight = jnp.where(own_here, own_weight, 0.0).T
    own_high = own_weight.astype(BF)
    own_comb = jnp.concatenate([own_high, (own_weight - own_high.astype(F32)).astype(BF)], axis=0)

    c_state.wait()

    @pl.loop(0, rows, unroll=4)
    def _(s):
        block = st[s]
        high = block.astype(BF)
        st_split[s, 0:dk, :] = high
        st_split[s, dk : 2 * dk, :] = (block - high.astype(F32)).astype(BF)

    for c in c_mix:
        c.wait()
    fgain_row = row(fgain)
    for i in range(8):
        fgain8[i : i + 1, :] = fgain_row[:, i * wide2 : (i + 1) * wide2]
    total(tok_all, n_tp - 1, recv_sem.at[0]).wait()

    def gained(blocks, gain_row):
        values = jnp.concatenate(blocks, axis=1).astype(F32)
        squares = jnp.mean(values * values, axis=1, keepdims=True)
        return (values * gain_row).astype(BF), lax.rsqrt(squares + EPS)

    rows_in, scale = gained([tok_all[t] for t in range(n_tp)], row(mgain))
    projected = (dot(rows_in, proj_w[...]) * scale).astype(BF).astype(F32)
    query, key, value, gate = (projected[:, i * dk : (i + 1) * dk] for i in range(4))

    def unit(v):
        return v * lax.rsqrt(jnp.sum(v * v, axis=1, keepdims=True) + EPS)

    query = unit(query) * dk ** (-0.5)
    key = unit(key)

    def two_parts(v):
        high = v.astype(BF).astype(F32)
        return high, v - high

    k_high, k_low = two_parts(key)
    q_high, q_low = two_parts(query)
    for s0 in range(0, rows, 8):
        some = slice(s0, s0 + 8)
        left = jnp.concatenate([k_high[some], q_high[some], k_low[some], q_low[some]], axis=0).astype(BF)
        left = jnp.concatenate([left, left], axis=1)
        for i in range(8):
            s = s0 + i
            both = dot(left, st_split[s])
            k_read[s : s + 1, :] = both[i : i + 1] + both[16 + i : 17 + i]
            q_read[s : s + 1, :] = both[8 + i : 9 + i] + both[24 + i : 25 + i]
    wide = rows_in.astype(F32)
    beta = jax.nn.sigmoid(jnp.sum(wide * wb[...].astype(F32), axis=1, keepdims=True) * scale)
    decay_in = jnp.sum(wide * wd[...].astype(F32), axis=1, keepdims=True) * scale + dbias[0]
    softplus = jnp.maximum(decay_in, 0.0) + jnp.log(1.0 + jnp.exp(-jnp.abs(decay_in)))
    decay = jnp.exp(-dscale[0] * softplus)
    written = beta * (value - decay * k_read[...])
    read = decay * q_read[...] + jnp.sum(query * key, axis=1, keepdims=True) * written
    squares = jnp.mean(read * read, axis=1, keepdims=True)
    gated = (read * lax.rsqrt(squares + EPS) * row(hgain) * silu(gate)).astype(BF)
    partial = dot(gated, wo[...])
    own_partial = jnp.zeros((rows, width), F32)
    for t in range(n_tp):
        piece = partial[:, t * width : (t + 1) * width]
        mix_send[t] = piece.astype(BF)
        own_partial = jnp.where(tp == t, piece, own_partial)
    for d in far_first:
        to_row(mix_send.at[lax.rem(tp + d, n_tp)], mix_recv.at[d - 1], 1, d)

    key_t = key.T
    for s in range(rows):
        st[s] = decay[s : s + 1, :] * st[s] + key_t[:, s : s + 1] * written[s : s + 1, :]

    total(mix_recv, n_tp - 1, recv_sem.at[1]).wait()
    mixed = own_partial
    for d in range(n_tp - 1):
        mixed = mixed + mix_recv[d].astype(F32)
    resid = tok_all[tp].astype(F32) + mixed
    resid_b = resid.astype(BF)

    res_all[tp] = resid_b
    disp_send[...] = dot(onehot[...], resid_b).astype(BF).reshape(disp_send.shape)

    def to_all(src, dst, phase, sign):
        to_y = [lax.rem(y + 4 + sign * r, 4) * 4 for r in RO]
        to_x = [lax.rem(x + 4 + sign * r, 4) for r in RO]
        to_ep = [to_y[b] + to_x[e] for b in range(4) for e in range(4)]

        def send(a, c, i, dev_tp):
            seats = pl.ds(2 * i, 2)
            pltpu.make_async_remote_copy(
                src.at[a, c, seats], dst.at[a, core, seats], send_sem.at[phase], recv_sem.at[phase],
                device_id=(to_ep[i], dev_tp), device_id_type=MESH,
            ).start()

        @pl.loop(0, 7)
        def _(a):
            dev_tp = lax.rem(z + ring(a, 8), 8) * 2
            for i in range(16):
                for c in range(2):
                    send(a, c, i, dev_tp + c)

        for i in range(15):
            for c in range(2):
                send(7, c, i, 2 * z + c)
        send(7, 1 - core, 15, 2 * z + 1 - core)

    def all_sent(sem):
        as_many = sized.at[pl.ds(0, slots - 2)]
        return pltpu.make_async_copy(as_many, as_many, sem)

    pl.semaphore_wait(entered, n_ep - 1)
    to_all(disp_send, disp_recv, 2, 1)
    for d in far_first:
        to_row(res_all.at[tp], res_all.at[tp], 3, d)
    own_disp = dot(own_onehot, resid_b).astype(BF)

    for c in c_ex:
        c.wait()
    all_sent(recv_sem.at[2]).wait()
    own_block = lax.broadcasted_iota(jnp.int32, (rows, width), 0) // 2 == n_ep - 1
    blocks = [disp_recv[a, c] for a in range(8) for c in range(2)]
    for c in range(2):
        blocks[14 + c] = jnp.where(own_block & (core == c), own_disp, blocks[14 + c])
    gain_from = jnp.concatenate([fgain8[pl.ds(z_from[a], 1), :] for a in range(8)], axis=1)
    rows_in, scale = gained(blocks, gain_from)
    hidden = (silu(dot(rows_in, eg[...]) * scale) * (dot(rows_in, eu[...]) * scale)).astype(BF)
    results = dot(hidden, ed[...])
    for a in range(8):
        for c in range(2):
            back_send[a, c] = results[:, (2 * a + c) * width : (2 * a + c + 1) * width].astype(BF)
    own_back = jnp.where(core == 0, results[:, 14 * width : 15 * width], results[:, 15 * width : 16 * width])
    to_all(back_send, back_recv, 4, -1)

    for c in c_sh:
        c.wait()
    total(res_all, n_tp - 1, recv_sem.at[3]).wait()
    rows_in, scale = gained([res_all[t] for t in range(n_tp)], fgain_row)
    hidden_shared = (silu(dot_nt(rows_in, sg[...]) * scale) * (dot_nt(rows_in, su[...]) * scale)).astype(BF)
    shared = dot(hidden_shared, sd[...])
    own_shared = jnp.zeros((rows, width), F32)
    for t in range(n_tp):
        piece = shared[:, t * width : (t + 1) * width]
        sh_send[t] = piece.astype(BF)
        own_shared = jnp.where(tp == t, piece, own_shared)
    for d in far_first:
        to_row(sh_send.at[lax.rem(tp + d, n_tp)], sh_recv.at[d - 1], 5, d)
    own_routed = dot(own_comb, own_back.astype(BF))
    final = resid + own_shared + own_routed[0:rows] + own_routed[rows : 2 * rows]
    total(sh_recv, n_tp - 1, recv_sem.at[5]).wait()
    for d in range(n_tp - 1):
        final = final + sh_recv[d].astype(F32)
    all_sent(recv_sem.at[4]).wait()
    own_rows = lax.broadcasted_iota(jnp.int32, (slots, width), 0) // 2 == (14 + core) * n_ep + n_ep - 1
    arrived = jnp.where(own_rows, jnp.zeros((slots, width), BF), back_recv[...].reshape(slots, width))
    routed = dot(comb[...], arrived)
    out[...] = (final + routed[0:rows] + routed[rows : 2 * rows]).astype(BF)

    for phase, ref in ((0, tok_all), (1, mix_recv), (3, res_all), (5, sh_recv)):
        total(ref, n_tp - 1, send_sem.at[phase]).wait()
    for phase in (2, 4):
        all_sent(send_sem.at[phase]).wait()


def put_out(out_v, st, out, new_state, sem):
    rows = st.shape[0]
    step = rows // 4
    c_out = pltpu.make_async_copy(out_v, out, sem.at[1])
    for i in range(4):
        some = pl.ds(i * step, step)
        pltpu.make_async_copy(st.at[some], new_state.at[some, 0], sem.at[0]).start()
    c_out.start()
    pltpu.make_async_copy(st, new_state.at[:, 0], sem.at[0]).wait()
    c_out.wait()


def body(
    tokens, delta_state, mix_gain, w_query, w_key, w_value, w_outgate, w_beta, w_decay, decay_scale, decay_bias,
    head_gain, w_output, ffn_gain, route_ids, route_weights, expert_gate, expert_up, expert_down, shared_gate,
    shared_up, shared_down,
):
    rows, width = tokens.shape
    n_ep, n_tp = lax.axis_size("ep"), lax.axis_size("tp")
    model, dk = w_query.shape
    top = route_ids.shape[1]
    fe = expert_gate.shape[2]
    fs = shared_gate.shape[1]
    slots = 2 * n_ep * n_tp
    block = (n_tp, rows, width)
    spread = (8, 2, rows, width)
    V = pltpu.VMEM
    dma = pltpu.SemaphoreType.DMA
    on_chip = pl.BlockSpec(memory_space=pltpu.VMEM)
    in_hbm = pl.BlockSpec(memory_space=pltpu.HBM)
    out_v, st = pl.pallas_call(
        kernel,
        out_shape=(V(tokens.shape, tokens.dtype), V((rows, dk, dk), F32)),
        in_specs=[in_hbm] * 22,
        out_specs=(on_chip, on_chip),
        scratch_shapes=[
            V(block, BF),
            V((rows, 2 * dk, dk), BF),
            V((model, 4 * dk), BF),
            V((1, model), BF),
            V((1, model), BF),
            pltpu.SMEM((1,), F32),
            pltpu.SMEM((1,), F32),
            V((model,), BF),
            V((dk,), BF),
            V((dk, model), BF),
            V((model,), BF),
            V((8, 2 * width), F32),
            V((top, rows), jnp.int32),
            V((top, rows), F32),
            V((model, fe), BF),
            V((model, fe), BF),
            V((fe, model), BF),
            V((fs, model), BF),
            V((fs, model), BF),
            V((fs, model), BF),
            V(block, BF),
            V((n_tp - 1, rows, width), BF),
            V(spread, BF),
            V(spread, BF),
            V(block, BF),
            V(spread, BF),
            V(spread, BF),
            V(block, BF),
            V((n_tp - 1, rows, width), BF),
            V((slots, rows), BF),
            V((2 * rows, slots), BF),
            V((rows, dk), F32),
            V((rows, dk), F32),
            V((slots, width), BF),
            dma((19,)),
            dma((6,)),
            dma((6,)),
            pltpu.SemaphoreType.REGULAR,
        ],
        compiler_params=pltpu.CompilerParams(
            collective_id=0, has_side_effects=True, vmem_limit_bytes=48 * 1024 * 1024
        ),
        name="layer",
    )(*(v if v.size == 1 else pltpu.with_memory_space_constraint(v, pltpu.HBM) for v in (
        tokens, delta_state, mix_gain, w_query, w_key, w_value, w_outgate, w_beta.T, w_decay.T,
        decay_scale, decay_bias, head_gain, w_output, ffn_gain, route_ids.T,
        route_weights.T, expert_gate, expert_up, expert_down, shared_gate.T, shared_up.T, shared_down,
    )))
    out_v, st = (pltpu.with_memory_space_constraint(v, pltpu.VMEM) for v in (out_v, st))
    return pl.pallas_call(
        put_out,
        out_shape=(
            jax.ShapeDtypeStruct(tokens.shape, tokens.dtype),
            jax.ShapeDtypeStruct(delta_state.shape, delta_state.dtype),
        ),
        in_specs=[on_chip, on_chip],
        out_specs=(in_hbm, in_hbm),
        scratch_shapes=[dma((2,))],
        name="put_out",
    )(out_v, st)


def solution(mesh):
    return jax.shard_map(
        body,
        mesh=mesh,
        in_specs=(
            P("ep", "tp"),
            P("ep", "tp", None, None),
            P(),
            P(None, "tp"),
            P(None, "tp"),
            P(None, "tp"),
            P(None, "tp"),
            P(None, "tp"),
            P(None, "tp"),
            P("tp"),
            P("tp"),
            P(),
            P("tp", None),
            P(),
            P("ep", None),
            P("ep", None),
            P(("ep", "tp"), None, None),
            P(("ep", "tp"), None, None),
            P(("ep", "tp"), None, None),
            P(None, "tp"),
            P(None, "tp"),
            P("tp", None),
        ),
        out_specs=(P("ep", "tp"), P("ep", "tp", None, None)),
        check_vma=False,
    )
```

```python
import jax
import jax.numpy as jnp
from jax import lax
from jax.experimental import pallas as pl
from jax.experimental.pallas import tpu as pltpu
from jax.sharding import PartitionSpec as P

EPS = 1e-06
MESH = pl.DeviceIdType.MESH
BF = jnp.bfloat16
F32 = jnp.float32
NT = (((1,), (1,)), ((), ()))


def silu(v):
    return v * jax.nn.sigmoid(v)


def dot(a, b):
    return jnp.dot(a, b, preferred_element_type=F32)


def dot_nt(a, b):
    return lax.dot_general(a, b, NT, preferred_element_type=F32)


def row(ref):
    return ref[...].astype(F32).reshape(1, -1)


ZO = (4, 3, 5, 2, 6, 1, 7, 0)
RO = (2, 1, 3, 0)


def hops(place):
    a, i = place
    return min(ZO[a], 8 - ZO[a]) + sum(min(RO[k], 4 - RO[k]) for k in (i // 4, i % 4))


BY_HOPS = sorted(((a, i) for i in range(16) for a in range(8)), key=lambda place: -hops(place))[:-1]


def ring(i, n):
    half = i // 2
    return n // 2 + half - lax.rem(i, 2) * (2 * half + 1)


def kernel(
    tokens, state, mix_gain, w_query, w_key, w_value, w_outgate, w_beta, w_decay, decay_scale, decay_bias,
    head_gain, w_output, ffn_gain, ids, weights, e_gate, e_up, e_down, s_gate, s_up, s_down,
    out, st,
    tok_all, st_split, proj_w, wb, wd, dscale, dbias, mgain, hgain, wo, fgain, fgain8, idv, rwv, eg, eu, ed, sg, su, sd,
    mix_send, mix_recv, disp_send, disp_recv, res_all, back_send, back_recv, sh_send, sh_recv,
    onehot, comb, k_read, q_read, sized,
    local_sem, send_sem, recv_sem, entered,
):
    n_ep, n_tp = 16, 16
    ep, tp = lax.axis_index("ep"), lax.axis_index("tp")
    me = ep * n_tp + tp
    y, x = ep // 4, lax.rem(ep, 4)
    z, core = tp // 2, lax.rem(tp, 2)
    rows, width = tokens.shape
    dk = state.shape[2]
    top = ids.shape[0]
    slots = 2 * n_ep * n_tp
    wide2 = 2 * width

    barrier = pltpu.get_barrier_semaphore()
    far_first = [8, 9, 7, 10, 6, 11, 5, 12, 4, 13, 3, 14, 2, 15, 1]
    for d in far_first:
        pl.semaphore_signal(barrier, inc=1, device_id=(ep, lax.rem(tp + d, n_tp)), device_id_type=MESH)
    for d in far_first:
        pl.semaphore_signal(barrier, inc=1, device_id=(lax.rem(ep + d, n_ep), tp), device_id_type=MESH)

    fetches = []

    def fetch(src, dst):
        copy = pltpu.make_async_copy(src, dst, local_sem.at[len(fetches)])
        fetches.append(copy)
        copy.start()
        return copy

    def fetch_pieces(pieces, whole):
        sem = local_sem.at[len(fetches)]
        for src, dst in pieces:
            pltpu.make_async_copy(src, dst, sem).start()
        fetches.append(pltpu.make_async_copy(whole, whole, sem))
        return fetches[-1]

    c_tok = fetch(tokens, tok_all.at[tp])
    c_route = [fetch(ids, idv), fetch(weights, rwv)]
    c_state = fetch(state.at[:, 0], st)
    c_mix = [
        fetch(mix_gain, mgain), fetch(w_beta, wb), fetch(w_decay, wd), fetch(decay_scale, dscale),
        fetch(decay_bias, dbias), fetch(head_gain, hgain), fetch(ffn_gain, fgain),
    ]
    four = enumerate((w_query, w_key, w_value, w_outgate))
    c_mix.append(fetch_pieces([(w, proj_w.at[:, pl.ds(i * dk, dk)]) for i, w in four], proj_w))
    c_mix.append(fetch(w_output, wo))
    c_sh = [fetch(s_gate, sg), fetch(s_up, su), fetch(s_down, sd)]
    z_from = [lax.rem(z + 8 - ZO[a], 8) for a in range(8)]
    z_to = [lax.rem(z + ZO[a], 8) for a in range(8)]
    here = [pl.ds(a * wide2, wide2) for a in range(8)]
    from_z = [pl.ds(pl.multiple_of(v * wide2, wide2), wide2) for v in z_from]
    to_z = [pl.ds(pl.multiple_of(v * wide2, wide2), wide2) for v in z_to]
    c_ex = [
        fetch_pieces([(e_gate.at[0, from_z[a]], eg.at[here[a]]) for a in range(8)], eg),
        fetch_pieces([(e_up.at[0, from_z[a]], eu.at[here[a]]) for a in range(8)], eu),
        fetch_pieces([(e_down.at[0, :, to_z[a]], ed.at[:, here[a]]) for a in range(8)], ed),
    ]

    def total(ref, count, sem):
        return pltpu.make_async_copy(ref.at[pl.ds(0, count)], ref.at[pl.ds(0, count)], sem)

    def to_row(src, dst, phase, d):
        pltpu.make_async_remote_copy(
            src, dst, send_sem.at[phase], recv_sem.at[phase],
            device_id=(ep, lax.rem(tp + d, n_tp)), device_id_type=MESH,
        ).start()

    c_tok.wait()
    pl.semaphore_wait(barrier, n_ep + n_tp - 2)
    for d in far_first:
        to_row(tok_all.at[tp], tok_all.at[tp], 0, d)
    for d in range(1, n_ep):
        pl.semaphore_signal(entered, inc=1, device_id=(lax.rem(ep + d, n_ep), tp), device_id_type=MESH)

    for c in c_route:
        c.wait()
    lower = (
        lax.broadcasted_iota(jnp.int32, (rows, rows), 0) < lax.broadcasted_iota(jnp.int32, (rows, rows), 1)
    ).astype(BF)

    def placed(expert, seat):
        named = jnp.zeros(expert.shape, F32)
        weight = jnp.zeros(expert.shape, F32)
        for j in range(top):
            hit = idv[j : j + 1, :] == expert
            named = jnp.where(hit, 1.0, named)
            weight = jnp.where(hit, rwv[j : j + 1, :], weight)
        before = dot(named.astype(BF), lower)
        return (named > 0.5) & (before == seat.astype(F32)), weight

    slot = lax.broadcasted_iota(jnp.int32, (slots, rows), 0)
    pair = slot // 2
    seat = slot - 2 * pair
    off_x, off_y = ring(pair % 4, 4), ring((pair // 4) % 4, 4)
    off_z, slot_core = ring(pair // 32, 8), (pair // 16) % 2
    far_ep = ((y + off_y) % 4) * 4 + (x + off_x) % 4
    here, _ = placed(far_ep * n_tp + ((z + off_z) % 8) * 2 + slot_core, seat)
    onehot[...] = jnp.where(here, 1.0, 0.0).astype(BF)
    here, weight = placed(far_ep * n_tp + ((z + 8 - off_z) % 8) * 2 + slot_core, seat)
    weight = jnp.where(here, weight, 0.0).T
    high = weight.astype(BF)
    comb[0:rows, :] = high
    comb[rows : 2 * rows, :] = (weight - high.astype(F32)).astype(BF)
    pair_row = lax.broadcasted_iota(jnp.int32, (rows, rows), 0)
    own_here, own_weight = placed(jnp.full((rows, rows), 0, jnp.int32) + me, pair_row % 2)
    own_here = own_here & (pair_row // 2 == n_ep - 1)
    own_onehot = jnp.where(own_here, 1.0, 0.0).astype(BF)
    own_weight = jnp.where(own_here, own_weight, 0.0).T
    own_high = own_weight.astype(BF)
    own_comb = jnp.concatenate([own_high, (own_weight - own_high.astype(F32)).astype(BF)], axis=0)

    c_state.wait()

    @pl.loop(0, rows, unroll=4)
    def _(s):
        block = st[s]
        high = block.astype(BF)
        st_split[s, 0:dk, :] = high
        st_split[s, dk : 2 * dk, :] = (block - high.astype(F32)).astype(BF)

    for c in c_mix:
        c.wait()
    fgain_row = row(fgain)
    for i in range(8):
        fgain8[i : i + 1, :] = fgain_row[:, i * wide2 : (i + 1) * wide2]
    total(tok_all, n_tp - 1, recv_sem.at[0]).wait()

    def gained(blocks, gain_row):
        values = jnp.concatenate(blocks, axis=1).astype(F32)
        squares = jnp.mean(values * values, axis=1, keepdims=True)
        return (values * gain_row).astype(BF), lax.rsqrt(squares + EPS)

    rows_in, scale = gained([tok_all[t] for t in range(n_tp)], row(mgain))
    projected = (dot(rows_in, proj_w[...]) * scale).astype(BF).astype(F32)
    query, key, value, gate = (projected[:, i * dk : (i + 1) * dk] for i in range(4))

    def unit(v):
        return v * lax.rsqrt(jnp.sum(v * v, axis=1, keepdims=True) + EPS)

    query = unit(query) * dk ** (-0.5)
    key = unit(key)

    def two_parts(v):
        high = v.astype(BF).astype(F32)
        return high, v - high

    k_high, k_low = two_parts(key)
    q_high, q_low = two_parts(query)
    for s0 in range(0, rows, 8):
        some = slice(s0, s0 + 8)
        left = jnp.concatenate([k_high[some], q_high[some], k_low[some], q_low[some]], axis=0).astype(BF)
        left = jnp.concatenate([left, left], axis=1)
        for i in range(8):
            s = s0 + i
            both = dot(left, st_split[s])
            k_read[s : s + 1, :] = both[i : i + 1] + both[16 + i : 17 + i]
            q_read[s : s + 1, :] = both[8 + i : 9 + i] + both[24 + i : 25 + i]
    wide = rows_in.astype(F32)
    beta = jax.nn.sigmoid(jnp.sum(wide * wb[...].astype(F32), axis=1, keepdims=True) * scale)
    decay_in = jnp.sum(wide * wd[...].astype(F32), axis=1, keepdims=True) * scale + dbias[0]
    softplus = jnp.maximum(decay_in, 0.0) + jnp.log(1.0 + jnp.exp(-jnp.abs(decay_in)))
    decay = jnp.exp(-dscale[0] * softplus)
    written = beta * (value - decay * k_read[...])
    read = decay * q_read[...] + jnp.sum(query * key, axis=1, keepdims=True) * written
    squares = jnp.mean(read * read, axis=1, keepdims=True)
    gated = (read * lax.rsqrt(squares + EPS) * row(hgain) * silu(gate)).astype(BF)
    partial = dot(gated, wo[...])
    own_partial = jnp.zeros((rows, width), F32)
    for t in range(n_tp):
        piece = partial[:, t * width : (t + 1) * width]
        mix_send[t] = piece.astype(BF)
        own_partial = jnp.where(tp == t, piece, own_partial)
    for d in far_first:
        to_row(mix_send.at[lax.rem(tp + d, n_tp)], mix_recv.at[d - 1], 1, d)

    key_t = key.T
    for s in range(rows):
        st[s] = decay[s : s + 1, :] * st[s] + key_t[:, s : s + 1] * written[s : s + 1, :]

    total(mix_recv, n_tp - 1, recv_sem.at[1]).wait()
    mixed = own_partial
    for d in range(n_tp - 1):
        mixed = mixed + mix_recv[d].astype(F32)
    resid = tok_all[tp].astype(F32) + mixed
    resid_b = resid.astype(BF)

    res_all[tp] = resid_b
    disp_send[...] = dot(onehot[...], resid_b).astype(BF).reshape(disp_send.shape)

    def to_all(src, dst, phase, sign):
        to_y = [lax.rem(y + 4 + sign * r, 4) * 4 for r in RO]
        to_x = [lax.rem(x + 4 + sign * r, 4) for r in RO]
        to_ep = [to_y[b] + to_x[e] for b in range(4) for e in range(4)]

        def send(a, c, i, dev_tp):
            seats = pl.ds(2 * i, 2)
            pltpu.make_async_remote_copy(
                src.at[a, c, seats], dst.at[a, core, seats], send_sem.at[phase], recv_sem.at[phase],
                device_id=(to_ep[i], dev_tp), device_id_type=MESH,
            ).start()

        for a, i in BY_HOPS:
            for c in range(2):
                send(a, c, i, 2 * z_to[a] + c)
        send(7, 1 - core, 15, 2 * z + 1 - core)

    def all_sent(sem):
        as_many = sized.at[pl.ds(0, slots - 2)]
        return pltpu.make_async_copy(as_many, as_many, sem)

    pl.semaphore_wait(entered, n_ep - 1)
    to_all(disp_send, disp_recv, 2, 1)
    for d in far_first:
        to_row(res_all.at[tp], res_all.at[tp], 3, d)
    own_disp = dot(own_onehot, resid_b).astype(BF)

    for c in c_ex:
        c.wait()
    all_sent(recv_sem.at[2]).wait()
    own_block = lax.broadcasted_iota(jnp.int32, (rows, width), 0) // 2 == n_ep - 1
    blocks = [disp_recv[a, c] for a in range(8) for c in range(2)]
    for c in range(2):
        blocks[14 + c] = jnp.where(own_block & (core == c), own_disp, blocks[14 + c])
    gain_from = jnp.concatenate([fgain8[pl.ds(z_from[a], 1), :] for a in range(8)], axis=1)
    rows_in, scale = gained(blocks, gain_from)
    hidden = (silu(dot(rows_in, eg[...]) * scale) * (dot(rows_in, eu[...]) * scale)).astype(BF)
    results = dot(hidden, ed[...])
    for a in range(8):
        for c in range(2):
            back_send[a, c] = results[:, (2 * a + c) * width : (2 * a + c + 1) * width].astype(BF)
    own_back = jnp.where(core == 0, results[:, 14 * width : 15 * width], results[:, 15 * width : 16 * width])
    to_all(back_send, back_recv, 4, -1)

    for c in c_sh:
        c.wait()
    total(res_all, n_tp - 1, recv_sem.at[3]).wait()
    rows_in, scale = gained([res_all[t] for t in range(n_tp)], fgain_row)
    hidden_shared = (silu(dot_nt(rows_in, sg[...]) * scale) * (dot_nt(rows_in, su[...]) * scale)).astype(BF)
    shared = dot(hidden_shared, sd[...])
    own_shared = jnp.zeros((rows, width), F32)
    for t in range(n_tp):
        piece = shared[:, t * width : (t + 1) * width]
        sh_send[t] = piece.astype(BF)
        own_shared = jnp.where(tp == t, piece, own_shared)
    for d in far_first:
        to_row(sh_send.at[lax.rem(tp + d, n_tp)], sh_recv.at[d - 1], 5, d)
    own_routed = dot(own_comb, own_back.astype(BF))
    final = resid + own_shared + own_routed[0:rows] + own_routed[rows : 2 * rows]
    total(sh_recv, n_tp - 1, recv_sem.at[5]).wait()
    for d in range(n_tp - 1):
        final = final + sh_recv[d].astype(F32)
    all_sent(recv_sem.at[4]).wait()
    own_rows = lax.broadcasted_iota(jnp.int32, (slots, width), 0) // 2 == (14 + core) * n_ep + n_ep - 1
    arrived = jnp.where(own_rows, jnp.zeros((slots, width), BF), back_recv[...].reshape(slots, width))
    routed = dot(comb[...], arrived)
    out[...] = (final + routed[0:rows] + routed[rows : 2 * rows]).astype(BF)

    for phase, ref in ((0, tok_all), (1, mix_recv), (3, res_all), (5, sh_recv)):
        total(ref, n_tp - 1, send_sem.at[phase]).wait()
    for phase in (2, 4):
        all_sent(send_sem.at[phase]).wait()


def put_out(out_v, st, out, new_state, sem):
    rows = st.shape[0]
    step = rows // 4
    c_out = pltpu.make_async_copy(out_v, out, sem.at[1])
    for i in range(4):
        some = pl.ds(i * step, step)
        pltpu.make_async_copy(st.at[some], new_state.at[some, 0], sem.at[0]).start()
    c_out.start()
    pltpu.make_async_copy(st, new_state.at[:, 0], sem.at[0]).wait()
    c_out.wait()


def body(
    tokens, delta_state, mix_gain, w_query, w_key, w_value, w_outgate, w_beta, w_decay, decay_scale, decay_bias,
    head_gain, w_output, ffn_gain, route_ids, route_weights, expert_gate, expert_up, expert_down, shared_gate,
    shared_up, shared_down,
):
    rows, width = tokens.shape
    n_ep, n_tp = lax.axis_size("ep"), lax.axis_size("tp")
    model, dk = w_query.shape
    top = route_ids.shape[1]
    fe = expert_gate.shape[2]
    fs = shared_gate.shape[1]
    slots = 2 * n_ep * n_tp
    block = (n_tp, rows, width)
    spread = (8, 2, rows, width)
    V = pltpu.VMEM
    dma = pltpu.SemaphoreType.DMA
    on_chip = pl.BlockSpec(memory_space=pltpu.VMEM)
    in_hbm = pl.BlockSpec(memory_space=pltpu.HBM)
    out_v, st = pl.pallas_call(
        kernel,
        out_shape=(V(tokens.shape, tokens.dtype), V((rows, dk, dk), F32)),
        in_specs=[in_hbm] * 22,
        out_specs=(on_chip, on_chip),
        scratch_shapes=[
            V(block, BF),
            V((rows, 2 * dk, dk), BF),
            V((model, 4 * dk), BF),
            V((1, model), BF),
            V((1, model), BF),
            pltpu.SMEM((1,), F32),
            pltpu.SMEM((1,), F32),
            V((model,), BF),
            V((dk,), BF),
            V((dk, model), BF),
            V((model,), BF),
            V((8, 2 * width), F32),
            V((top, rows), jnp.int32),
            V((top, rows), F32),
            V((model, fe), BF),
            V((model, fe), BF),
            V((fe, model), BF),
            V((fs, model), BF),
            V((fs, model), BF),
            V((fs, model), BF),
            V(block, BF),
            V((n_tp - 1, rows, width), BF),
            V(spread, BF),
            V(spread, BF),
            V(block, BF),
            V(spread, BF),
            V(spread, BF),
            V(block, BF),
            V((n_tp - 1, rows, width), BF),
            V((slots, rows), BF),
            V((2 * rows, slots), BF),
            V((rows, dk), F32),
            V((rows, dk), F32),
            V((slots, width), BF),
            dma((19,)),
            dma((6,)),
            dma((6,)),
            pltpu.SemaphoreType.REGULAR,
        ],
        compiler_params=pltpu.CompilerParams(
            collective_id=0, has_side_effects=True, vmem_limit_bytes=48 * 1024 * 1024
        ),
        name="layer",
    )(*(v if v.size == 1 else pltpu.with_memory_space_constraint(v, pltpu.HBM) for v in (
        tokens, delta_state, mix_gain, w_query, w_key, w_value, w_outgate, w_beta.T, w_decay.T,
        decay_scale, decay_bias, head_gain, w_output, ffn_gain, route_ids.T,
        route_weights.T, expert_gate, expert_up, expert_down, shared_gate.T, shared_up.T, shared_down,
    )))
    out_v, st = (pltpu.with_memory_space_constraint(v, pltpu.VMEM) for v in (out_v, st))
    return pl.pallas_call(
        put_out,
        out_shape=(
            jax.ShapeDtypeStruct(tokens.shape, tokens.dtype),
            jax.ShapeDtypeStruct(delta_state.shape, delta_state.dtype),
        ),
        in_specs=[on_chip, on_chip],
        out_specs=(in_hbm, in_hbm),
        scratch_shapes=[dma((2,))],
        name="put_out",
    )(out_v, st)


def solution(mesh):
    return jax.shard_map(
        body,
        mesh=mesh,
        in_specs=(
            P("ep", "tp"),
            P("ep", "tp", None, None),
            P(),
            P(None, "tp"),
            P(None, "tp"),
            P(None, "tp"),
            P(None, "tp"),
            P(None, "tp"),
            P(None, "tp"),
            P("tp"),
            P("tp"),
            P(),
            P("tp", None),
            P(),
            P("ep", None),
            P("ep", None),
            P(("ep", "tp"), None, None),
            P(("ep", "tp"), None, None),
            P(("ep", "tp"), None, None),
            P(None, "tp"),
            P(None, "tp"),
            P("tp", None),
        ),
        out_specs=(P("ep", "tp"), P("ep", "tp", None, None)),
        check_vma=False,
    )
```
